256 devices in a mesh: ep: 64 (over z, x, core), tp: 4 (over y).
Axes of the slice: x: 4, y: 4, z: 8, core: 2. Of those that a mesh axis runs over, the one named last changes fastest.
Arguments:
- queries: bfloat16 [16384, 8, 128], P('ep', 'tp'), may hold values from -256 to 256
- keys: bfloat16 [16384, 4, 128], P('ep', 'tp'), may hold values from -8 to 8
- values: bfloat16 [16384, 4, 128], P('ep', 'tp'), may hold values from -6 to 6
- attn_lambda: float32 [8], P('tp'), may hold values from 0.3 to 0.8
- head_gain: float32 [128], replicated, may hold values from 0.1 to 1.9
- w_out: bfloat16 [1024, 2048], replicated, may hold values from -0.1875 to 0.1875
- moe_rows: bfloat16 [32768, 2048], P('ep'), may hold values from -6 to 6
- moe_gain: float32 [2048], replicated, may hold values from 0.1 to 1.9
- routes: int32 [32768, 2], P('ep'), may hold values from 0 to 63, all different within a row; in each aligned block of 128 rows (0 to 127, 128 to 255, ...) at most 8 rows name the same one
- route_weights: float32 [32768, 2], P('ep'), may hold values from 0.1 to 1
- w_gate: bfloat16 [64, 2048, 1024], P('ep', None, 'tp'), may hold values from -0.125 to 0.125
- w_up: bfloat16 [64, 2048, 1024], P('ep', None, 'tp'), may hold values from -0.125 to 0.125
- w_down: bfloat16 [64, 1024, 2048], P('ep', 'tp'), may hold values from -0.1875 to 0.1875
Outputs:
- mixer_out: bfloat16 [16384, 2048], P(('ep', 'tp'))
- moe_out: bfloat16 [32768, 2048], P(('ep', 'tp'))
The draws below stay inside these ranges and needn't reach their ends.
Inputs may be any that keep to these rules, and one draw needn't show every extreme that they name: `routes`: each row names 2 different experts. In each aligned block of 128 rows (the rows of moe_out that one device holds) no expert is named by more than 8 rows, a bound that some block reaches.
All inputs are finite; a program needn't handle non-finite values.
Results may differ from the reference program's by a relative error of at most 0.011.
Values may be sent and summed in bfloat16 or wider, within the bound.
A program may use at most 128 MiB of HBM per device.

```python
import math
import jax
import jax.numpy as jnp
import numpy as np
from jax import lax

D = 2048
HQ = 8
KVH = 4
HEAD = 64
VDIM = 128
FF = 1024
TOPK = 2
MOE_DEV = 128
EXPERTS = 64
CAP = 8
ATT_TOKENS = 16384
MOE_TOKENS = 32768
N_EP = 64
N_TP = 4


def pair_draw(key):
    spread = 1.75 ** 0.5
    base_q = jax.random.truncated_normal(jax.random.fold_in(key, 101), -4.5, 4.5, (ATT_TOKENS, HQ, 2, HEAD), jnp.float32) * spread
    base_k = jax.random.truncated_normal(jax.random.fold_in(key, 102), -4.5, 4.5, (ATT_TOKENS, KVH, 2, HEAD), jnp.float32) * spread
    return (base_q.reshape(ATT_TOKENS, HQ, 2 * HEAD), base_k.reshape(ATT_TOKENS, KVH, 2 * HEAD))


def draw_queries(key, part):
    return pair_draw(key)[0].astype(jnp.bfloat16)


def draw_keys(key, part):
    return pair_draw(key)[1].astype(jnp.bfloat16)


def steps_of(key, shape, shards, low, high):
    factor_of = 1.0
    for dim, blocks in shards:
        steps = jax.random.uniform(jax.random.fold_in(jax.random.fold_in(key, 6), dim), (blocks,), jnp.float32, low / len(shards), high / len(shards))
        factor_of = factor_of * jnp.repeat(jnp.exp(steps), shape[dim] // blocks).reshape((-1,) + (1,) * (len(shape) - 1 - dim))
    return factor_of


def deal_out(key, own, number, rows, number_of, top, limit, slope):
    order = jax.random.permutation(key, number_of)
    heavy_load, ordinary = load_shares(number_of, rows * top, limit, slope, True), load_shares(number_of, rows * top, limit, slope, False)
    places = jnp.arange(number_of)

    def named(tallies, offset_by):
        used = int((tallies > 0).sum())
        fixed = max(1, used // 4)
        moved = fixed + (places - fixed + offset_by * (used - fixed)) % max(1, number_of - fixed)
        return jnp.zeros((number_of,), jnp.int32).at[order[jnp.where(places < fixed, places, moved)]].set(jnp.asarray(tallies, jnp.int32))

    tallies = jnp.where(number % 4 == 0, named(heavy_load, number // 4), named(ordinary, number - number // 4 - 1))
    mixed = jax.random.permutation(jax.random.fold_in(own, 3), number_of)
    source_of, taker = mixed[0:number_of // 2 * 2:2], mixed[1:number_of // 2 * 2:2]
    slack = jnp.minimum(tallies[source_of] - 1, limit - tallies[taker]) // 2
    slack = jnp.where((source_of == order[0]) | (taker == order[0]) | (tallies[taker] == 0), 0, jnp.maximum(slack, 0))
    moved = jax.random.randint(jax.random.fold_in(own, 4), (number_of // 2,), 0, 1 << 20) % (slack + 1)
    tallies = tallies.at[source_of].add(-moved).at[taker].add(moved)
    members = jnp.searchsorted(jnp.cumsum(tallies), jnp.arange(rows * top), side="right").astype(jnp.int32)
    table = members.reshape(top, rows).T
    table = table[jax.random.permutation(jax.random.fold_in(own, 1), rows)]
    offset_by = jax.random.randint(jax.random.fold_in(own, 2), (rows, 1), 0, top)
    return jnp.take_along_axis(table, (jnp.arange(top)[None, :] + offset_by) % top, axis=1)


def load_shares(amount, total, bound, lean, full):
    weights = [(1 << 20) // math.isqrt(standing ** lean) + 1 for standing in range(1, amount + 1)]
    largest = bound if full else min(bound, max(-(-total // amount), total * weights[0] // sum(weights)))
    least = 1 if total - largest >= amount - 1 else 0
    counts, spare = [largest] + [least] * (amount - 1), total - largest - least * (amount - 1)
    while spare > 0:
        free = [i for i in range(1, amount) if counts[i] < largest] or [i for i in range(1, amount) if counts[i] < bound]
        pool, budget = sum([weights[i] for i in free]), spare
        for i in free:
            extra = min(bound - counts[i], max(1, budget * weights[i] // pool), spare)
            counts[i] = counts[i] + extra
            spare = spare - extra
    return np.array(counts)


def normal_values(rng, extent, deviation, limit, split=(), kind=jnp.bfloat16):
    entries = deviation * jax.random.normal(rng, extent, jnp.float32)
    if split:
        entries = entries * steps_of(rng, extent, split, -0.22, 0.18)
    return jnp.clip(entries, -limit, limit).astype(kind)


def setup_inputs(seed: int = 0) -> dict:
    streams_of = jax.random.split(jax.random.key(seed), 14)
    queries = draw_queries(jax.random.fold_in(streams_of[13], 71), 0)
    keys = draw_keys(jax.random.fold_in(streams_of[13], 71), 0)
    values = normal_values(streams_of[2], (ATT_TOKENS, KVH, VDIM), 1.0, 6.0, ((0, 64), (1, 4)))
    attn_lambda = jnp.clip(0.3 + 0.5 * jax.random.uniform(streams_of[3], (HQ,), jnp.float32) ** steps_of(streams_of[3], (HQ,), ((0, 4),), -0.2, 0.2), 0.3, 0.8)
    head_gain = jnp.clip(1.0 + 0.18 * jax.random.normal(streams_of[4], (VDIM,), jnp.float32), 0.1, 1.9)
    w_out = normal_values(streams_of[5], (HQ * VDIM, D), (HQ * VDIM) ** -0.5, 0.1875)
    moe_rows = normal_values(streams_of[6], (MOE_TOKENS, D), 1.0, 6.0, ((0, 64),))
    moe_gain = jnp.clip(1.0 + 0.18 * jax.random.normal(streams_of[7], (D,), jnp.float32), 0.1, 1.9)
    routes_keys = jax.random.split(jax.random.fold_in(streams_of[8], 1), MOE_TOKENS // MOE_DEV)
    routes_turns = jax.random.permutation(jax.random.fold_in(streams_of[8], 3), MOE_TOKENS // MOE_DEV)
    routes = jax.vmap(lambda own, number: deal_out(jax.random.fold_in(streams_of[8], 2), own, number, MOE_DEV, EXPERTS, TOPK, CAP, 1))(routes_keys, routes_turns).reshape((MOE_TOKENS, TOPK))
    route_weights = jnp.clip(0.1 + 0.9 * jax.random.uniform(streams_of[9], (MOE_TOKENS, TOPK), jnp.float32) ** steps_of(streams_of[9], (MOE_TOKENS, TOPK), ((0, 64),), -0.2, 0.2), 0.1, 1.0)
    w_gate = normal_values(streams_of[10], (EXPERTS, D, FF), D ** -0.5, 0.125, ((0, 64), (2, 4)))
    w_up = normal_values(streams_of[11], (EXPERTS, D, FF), D ** -0.5, 0.125, ((0, 64), (2, 4)))
    w_down = normal_values(streams_of[12], (EXPERTS, FF, D), FF ** -0.5, 0.1875, ((0, 64), (1, 4)))
    return dict(queries=queries, keys=keys, values=values, attn_lambda=attn_lambda, head_gain=head_gain, w_out=w_out, moe_rows=moe_rows, moe_gain=moe_gain, routes=routes, route_weights=route_weights, w_gate=w_gate, w_up=w_up, w_down=w_down)


EPSILON = 1e-06
MASKED = -1e+30

def reference(queries, keys, values, attn_lambda, head_gain, w_out, moe_rows, moe_gain, routes, route_weights, w_gate, w_up, w_down):
    length = queries.shape[0]
    per_key = HQ // KVH
    key_all = jnp.repeat(keys.astype(jnp.float32).reshape(length, KVH, 2, HEAD), per_key, axis=1)
    value_all = jnp.repeat(values.astype(jnp.float32), per_key, axis=1)
    block_len = math.gcd(length, 256)
    block_count = length // block_len
    query_all = queries.astype(jnp.float32).reshape(block_count, block_len, HQ, 2, HEAD)
    key_pos = jnp.arange(length, dtype=jnp.int32)

    def one_block(inputs):
        query_blk, block_index = inputs
        query_pos = block_index * block_len + jnp.arange(block_len, dtype=jnp.int32)
        scores = jnp.einsum('qhmd,khmd->hmqk', query_blk, key_all) * HEAD ** (-0.5)
        allowed = key_pos[None, :] <= query_pos[:, None]
        scores = jnp.where(allowed, scores, MASKED)
        row_max = lax.optimization_barrier(jnp.max(scores, axis=-1, keepdims=True))
        weights = jnp.exp(scores - row_max)
        totals = lax.optimization_barrier(jnp.sum(weights, axis=-1))
        rounded = lax.optimization_barrier(weights.astype(jnp.bfloat16)).astype(jnp.float32)
        numerator = jnp.einsum('hmqk,khv->hmqv', rounded, value_all)
        ratios = numerator / totals[..., None]
        head_out = ratios[:, 0] - attn_lambda[:, None, None] * ratios[:, 1]
        inv_rms = lax.rsqrt(lax.optimization_barrier(jnp.mean(head_out * head_out, axis=-1, keepdims=True)) + EPSILON)
        normed_heads = (head_out * inv_rms * head_gain).astype(jnp.bfloat16)
        return jnp.transpose(normed_heads, (1, 0, 2)).reshape(block_len, HQ * VDIM)
    attn_rows = lax.map(one_block, (query_all, jnp.arange(block_count, dtype=jnp.int32)))
    attn_rows = attn_rows.reshape(length, HQ * VDIM)
    mixer_out = jnp.dot(attn_rows, w_out, preferred_element_type=jnp.float32).astype(jnp.bfloat16)
    rows_f = moe_rows.astype(jnp.float32)
    normed = (rows_f * lax.rsqrt(lax.optimization_barrier(jnp.mean(rows_f * rows_f, axis=-1, keepdims=True)) + EPSILON) * moe_gain).astype(jnp.bfloat16)
    tokens = moe_rows.shape[0]
    pairs = tokens * TOPK
    flat_ids = routes.reshape(-1).astype(jnp.int32)
    matches = (flat_ids[:, None] == jnp.arange(EXPERTS, dtype=jnp.int32)[None, :]).astype(jnp.int32)
    earlier = jnp.cumsum(matches, axis=0) - matches
    position = lax.optimization_barrier(jnp.sum(earlier * matches, axis=1)).astype(jnp.int32)
    slot_total = N_EP * N_TP * CAP
    pair_table = jnp.full((EXPERTS, slot_total), pairs, dtype=jnp.int32)
    pair_table = pair_table.at[flat_ids, position].set(jnp.arange(pairs, dtype=jnp.int32))
    token_table = jnp.where(pair_table < pairs, pair_table // TOPK, tokens).astype(jnp.int32)
    weight_flat = jnp.concatenate([route_weights.reshape(-1), jnp.zeros((1,), jnp.float32)])
    weight_table = weight_flat[pair_table]
    padded = jnp.concatenate([normed, jnp.zeros((1, D), jnp.bfloat16)], axis=0)
    group_width = FF // N_TP

    def one_expert(accumulated, inputs):
        token_row, weight_row, gate_w, up_w, down_w = inputs
        chosen = padded[token_row]
        gate_out = jnp.dot(chosen, gate_w, preferred_element_type=jnp.float32)
        up_out = jnp.dot(chosen, up_w, preferred_element_type=jnp.float32)
        hidden = (jax.nn.silu(gate_out) * up_out).astype(jnp.bfloat16)
        partials = jnp.einsum('stf,tfd->tsd', hidden.reshape(slot_total, N_TP, group_width).astype(jnp.float32), down_w.reshape(N_TP, group_width, D).astype(jnp.float32))
        partials = lax.optimization_barrier(partials.astype(jnp.bfloat16)).astype(jnp.float32)
        expert_out = lax.optimization_barrier(lax.optimization_barrier(jnp.sum(partials, axis=0)).astype(jnp.bfloat16)).astype(jnp.float32)
        accumulated = accumulated.at[token_row].add(weight_row[:, None] * expert_out)
        return (accumulated, None)
    start_total = jnp.zeros((tokens + 1, D), jnp.float32)
    accumulated, unused = lax.scan(one_expert, start_total, (token_table, weight_table, w_gate, w_up, w_down))
    moe_out = accumulated[:tokens].astype(jnp.bfloat16)
    return (mixer_out, moe_out)
```

```python
import functools

import jax
import jax.numpy as jnp
from jax import lax
from jax.experimental import pallas as pl
from jax.experimental.pallas import tpu as pltpu
from jax.sharding import PartitionSpec as P

EPSILON = 1e-06
MASKED = -1e30
MESH = pl.DeviceIdType.MESH
CAP = 8
BF = jnp.bfloat16
F32 = jnp.float32
ANY = pl.BlockSpec(memory_space=pl.ANY)
VM = pl.BlockSpec(memory_space=pltpu.VMEM)


def one_hot_slots(route_a, route_b, shape, token_dim, counts):
    slot_dim = 1 - token_dim
    slot = lax.broadcasted_iota(jnp.int32, shape, slot_dim)
    expert = slot // CAP
    place = (slot - expert * CAP).astype(F32)
    hit_a, hit_b = route_a == expert, route_b == expert
    hit = (hit_a | hit_b).astype(F32).astype(BF)
    earlier = counts(hit)
    here = earlier == place
    return hit_a & here, hit_b & here


def pack_kernel(rows_ref, gain_ref, routes_ref, out_ref):
    tokens = rows_ref.shape[0]
    slots = out_ref.shape[0]
    rows = rows_ref[...].astype(F32)
    mean_sq = jnp.mean(rows * rows, axis=-1, keepdims=True)
    normed = (rows * lax.rsqrt(mean_sq + EPSILON) * gain_ref[...]).astype(BF)
    before = (
        lax.broadcasted_iota(jnp.int32, (tokens, tokens), 0)
        < lax.broadcasted_iota(jnp.int32, (tokens, tokens), 1)
    )
    before = before.astype(F32).astype(BF)

    def counts(hit):
        return jnp.dot(hit, before, preferred_element_type=F32)

    first, second = one_hot_slots(
        routes_ref[0:1, :], routes_ref[1:2, :], (slots, tokens), 1, counts
    )
    pick = (first | second).astype(F32).astype(BF)
    step = 256
    for n in range(0, rows_ref.shape[1], step):
        out_ref[:, n : n + step] = jnp.dot(
            pick, normed[:, n : n + step], preferred_element_type=F32
        ).astype(BF)


def combine_kernel(back_ref, routes_ref, weights_ref, out_ref):
    tokens = out_ref.shape[0]
    slots = back_ref.shape[0]
    before = (
        lax.broadcasted_iota(jnp.int32, (tokens, tokens), 1)
        < lax.broadcasted_iota(jnp.int32, (tokens, tokens), 0)
    )
    before = before.astype(F32).astype(BF)

    def counts(hit):
        return jnp.dot(before, hit, preferred_element_type=F32)

    first, second = one_hot_slots(
        routes_ref[:, 0:1], routes_ref[:, 1:2], (tokens, slots), 0, counts
    )
    mix = jnp.where(first, weights_ref[:, 0:1], 0.0) + jnp.where(second, weights_ref[:, 1:2], 0.0)
    high = mix.astype(BF)
    low = (mix - high.astype(F32)).astype(BF)
    step = 256
    for n in range(0, out_ref.shape[1], step):
        part = back_ref[:, n : n + step]
        out_ref[:, n : n + step] = (
            jnp.dot(high, part, preferred_element_type=F32)
            + jnp.dot(low, part, preferred_element_type=F32)
        ).astype(BF)


def comm_kernel(
    n_ep, n_tp, nz, nx,
    slots_ref, kv_ref, wg_ref, wu_ref, wd_ref,
    arrived_ref, kv_all_ref, g_ref, u_ref, d_ref,
    slot_tmp, kv_tmp, w_tmp, wd_tmp,
    w_send, w_recv, f_send, f_recv, z_send, z_recv, x_send, x_recv, y_send, y_recv,
    c_send, c_recv, d_send, d_recv, local_sem,
):
    me = lax.axis_index("ep")
    tp = lax.axis_index("tp")
    z = me // (2 * nx)
    x = (me // 2) % nx
    c = me % 2

    def ep_of(zz, xx, cc):
        return zz * (2 * nx) + xx * 2 + cc

    barrier = pltpu.get_barrier_semaphore()

    def greet(d, carry):
        pl.semaphore_signal(
            barrier, inc=1, device_id={"ep": lax.rem(me + d, n_ep)}, device_id_type=MESH
        )
        return carry

    lax.fori_loop(1, n_ep, greet, 0)
    for d in range(1, n_tp):
        pl.semaphore_signal(
            barrier, inc=1, device_id={"tp": lax.rem(tp + d, n_tp)}, device_id_type=MESH
        )
    pl.semaphore_wait(barrier, n_ep - 1 + n_tp - 1)

    def remote(src, dst, send, recv, where):
        return pltpu.make_async_remote_copy(
            src_ref=src, dst_ref=dst, send_sem=send, recv_sem=recv,
            device_id=where, device_id_type=MESH,
        )

    up, down = {"tp": lax.rem(tp + 1, n_tp)}, {"tp": lax.rem(tp + n_tp - 1, n_tp)}
    pairs = ((wg_ref, g_ref), (wu_ref, u_ref), (wd_ref, d_ref))

    def z_copy(k):
        to = ep_of(lax.rem(z + k, nz), x, c)
        return remote(kv_ref, kv_all_ref.at[z, x, c], z_send.at[k], z_recv.at[k], {"ep": to})

    for k in range(1, nz):
        z_copy(k).start()
    weights = []
    for i, (src, dst) in enumerate(pairs):
        for s, where in enumerate((up, down)):
            w = remote(src, dst.at[tp], w_send.at[s, i], w_recv.at[s, i], where)
            w.start()
            weights.append(w)

    def row_copy(d):
        to = lax.rem(me + d, n_ep)
        return remote(
            slots_ref.at[to], arrived_ref.at[me], d_send.at[d], d_recv.at[d], {"ep": to}
        )

    def row_start(d, carry):
        row_copy(d).start()
        return carry

    half = n_ep // 2
    lax.fori_loop(1, half, row_start, 0)

    def stay(src, tmp, dst, n):
        pull = pltpu.make_async_copy(src, tmp, local_sem.at[n])
        pull.start()
        pull.wait()
        push = pltpu.make_async_copy(tmp, dst, local_sem.at[n])
        push.start()
        push.wait()

    stay(kv_ref, kv_tmp, kv_all_ref.at[z, x, c], 0)
    stay(slots_ref.at[me], slot_tmp, arrived_ref.at[me], 1)
    stay(wg_ref, w_tmp, g_ref.at[tp], 2)
    stay(wu_ref, w_tmp, u_ref.at[tp], 2)
    stay(wd_ref, wd_tmp, d_ref.at[tp], 3)

    for k in range(1, nz):
        z_copy(k).wait()

    xr, xl = lax.rem(x + 1, nx), lax.rem(x + nx - 1, nx)
    x2 = lax.rem(x + 2, nx)
    right, left = {"ep": ep_of(z, xr, c)}, {"ep": ep_of(z, xl, c)}
    twin = {"ep": ep_of(z, x, 1 - c)}

    def column(xx):
        return kv_all_ref.at[:, xx, c]

    def across(n, xx):
        return remote(column(xx), column(xx), c_send.at[n], c_recv.at[n], twin)

    to_right = remote(column(x), column(x), x_send.at[0], x_recv.at[0], right)
    to_left = remote(column(x), column(x), x_send.at[1], x_recv.at[1], left)
    to_right.start()
    to_left.start()
    across(0, x).start()
    lax.fori_loop(half, n_ep, row_start, 0)

    def forward(i):
        src, dst = pairs[i]
        mid = src.shape[0] // 2
        came_up, came_down = lax.rem(tp + n_tp - 1, n_tp), lax.rem(tp + 1, n_tp)
        low, high = pl.ds(0, mid), pl.ds(mid, mid)
        return (
            remote(dst.at[came_up, low], dst.at[came_up, low], f_send.at[0, i], f_recv.at[0, i], up),
            remote(
                dst.at[came_down, high], dst.at[came_down, high], f_send.at[1, i], f_recv.at[1, i], down
            ),
        )

    def pass_on(i):
        for w in weights[2 * i : 2 * i + 2]:
            w.wait_recv()
        for f in forward(i):
            f.start()

    pass_on(0)
    pass_on(1)

    to_right.wait_recv()
    hz = nz // 2
    on_right = remote(
        kv_all_ref.at[pl.ds(0, hz), xl, c], kv_all_ref.at[pl.ds(0, hz), xl, c],
        y_send.at[0], y_recv.at[0], right,
    )
    on_right.start()
    across(1, xl).start()
    to_left.wait_recv()
    on_left = remote(
        kv_all_ref.at[pl.ds(hz, hz), xr, c], kv_all_ref.at[pl.ds(hz, hz), xr, c],
        y_send.at[1], y_recv.at[1], left,
    )
    on_left.start()
    across(2, xr).start()
    pass_on(2)
    on_right.wait_recv()
    on_left.wait_recv()
    across(3, x2).start()

    def row_wait(d, carry):
        row_copy(d).wait()
        return carry

    lax.fori_loop(1, n_ep, row_wait, 0)
    for n, xx in enumerate((x, xl, xr, x2)):
        across(n, xx).wait()
    for w in weights:
        w.wait_send()
    for i in range(3):
        for f in forward(i):
            f.wait()
    for w in (to_right, to_left, on_right, on_left):
        w.wait_send()


def expert_kernel(rows_ref, g_ref, u_ref, d_ref, out_ref, acc_ref):
    g = pl.program_id(0)

    @pl.when(g == 0)
    def _():
        acc_ref[...] = jnp.zeros_like(acc_ref)

    step = 256
    for m in range(0, rows_ref.shape[0], step):
        rows = rows_ref[m : m + step, :]
        gate = jnp.dot(rows, g_ref[0], preferred_element_type=F32)
        upper = jnp.dot(rows, u_ref[0], preferred_element_type=F32)
        hidden = (gate / (1.0 + jnp.exp(-gate)) * upper).astype(BF)
        for n in range(0, out_ref.shape[1], 512):
            part = jnp.dot(hidden, d_ref[0, :, n : n + 512], preferred_element_type=F32)
            acc_ref[m : m + step, n : n + 512] += part.astype(BF).astype(F32)

    @pl.when(g == pl.num_programs(0) - 1)
    def _():
        out_ref[...] = acc_ref[...].astype(BF)


def attention_kernel(blk, q_ref, kv_ref, lam_ref, gain_ref, out_ref, q_s, m_s, acc_s):
    me = lax.axis_index("ep")
    rows = q_ref.shape[1]
    heads = q_ref.shape[0]
    vdim = q_ref.shape[2]
    hd = vdim // 2
    lane = lax.broadcasted_iota(jnp.int32, (rows, vdim), 1)
    for h in range(heads):
        q = q_ref[h] * jnp.asarray(hd**-0.5, BF)
        for m in range(2):
            q_s[2 * h + m] = jnp.where((lane // hd) == m, q, jnp.zeros_like(q))
    m_s[...] = jnp.full_like(m_s, MASKED)
    acc_s[...] = jnp.zeros_like(acc_s)

    def block(b, masked):
        start = pl.multiple_of(b * blk, blk)
        k = kv_ref[pl.ds(start, blk), 0:vdim]
        v = kv_ref[pl.ds(start, blk), vdim : 2 * vdim]
        v_one = jnp.concatenate([v, jnp.ones_like(v)], axis=1)
        for r in range(2 * heads):
            s = lax.dot_general(
                q_s[r], k, (((1,), (1,)), ((), ())), preferred_element_type=F32
            )
            if masked:
                kp = start + lax.broadcasted_iota(jnp.int32, s.shape, 1)
                qp = me * rows + lax.broadcasted_iota(jnp.int32, s.shape, 0)
                s = jnp.where(kp <= qp, s, MASKED)
            old = m_s[r]
            new = jnp.maximum(old, jnp.max(s, axis=1, keepdims=True))
            shrink = jnp.exp(old - new)
            p = jnp.exp(s - new[:, 0:1]).astype(BF)
            m_s[r] = new
            acc_s[r] = acc_s[r] * shrink[:, 0:1] + jnp.dot(p, v_one, preferred_element_type=F32)

    last = (me * rows) // blk

    def body(b, carry):
        block(b, False)
        return carry

    lax.fori_loop(0, last, body, 0)
    block(last, True)
    for h in range(heads):
        ratio = [acc_s[2 * h + m][:, 0:vdim] / acc_s[2 * h + m][:, vdim:] for m in range(2)]
        out = ratio[0] - lam_ref[h] * ratio[1]
        mean_sq = jnp.mean(out * out, axis=-1, keepdims=True)
        out_ref[:, h * vdim : (h + 1) * vdim] = (
            out * lax.rsqrt(mean_sq + EPSILON) * gain_ref[...]
        ).astype(BF)


def params(**kw):
    return pltpu.CompilerParams(vmem_limit_bytes=48 * 1024 * 1024, **kw)


def local(
    queries, keys, values, attn_lambda, head_gain, w_out,
    moe_rows, moe_gain, routes, route_weights, w_gate, w_up, w_down,
):
    n_ep, n_tp = lax.axis_size("ep"), lax.axis_size("tp")
    nx = 4
    nz = n_ep // (2 * nx)
    tp = lax.axis_index("tp")
    positions, heads, vdim = queries.shape
    width = moe_rows.shape[1]
    dev_rows = moe_rows.shape[0] // n_tp
    slots = n_ep * CAP
    hid = w_gate.shape[2]

    own_rows = lax.dynamic_slice_in_dim(moe_rows, tp * dev_rows, dev_rows, 0)
    own_routes = lax.dynamic_slice_in_dim(routes, tp * dev_rows, dev_rows, 0)
    own_weights = lax.dynamic_slice_in_dim(route_weights, tp * dev_rows, dev_rows, 0)

    outgoing = pl.pallas_call(
        pack_kernel,
        out_shape=jax.ShapeDtypeStruct((slots, width), BF),
        in_specs=[VM, VM, VM],
        out_specs=VM,
        compiler_params=params(),
        name="pack",
    )(own_rows, moe_gain.reshape(1, width), own_routes.T)

    kv = jnp.concatenate([keys[:, 0], values[:, 0]], axis=1)
    sem = pltpu.SemaphoreType.DMA
    arrived, kv_all, g_all, u_all, d_all = pl.pallas_call(
        functools.partial(comm_kernel, n_ep, n_tp, nz, nx),
        out_shape=[
            jax.ShapeDtypeStruct((n_ep, CAP, width), BF),
            jax.ShapeDtypeStruct((nz, nx, 2, positions, 2 * vdim), BF),
            jax.ShapeDtypeStruct((n_tp, width, hid), BF),
            jax.ShapeDtypeStruct((n_tp, width, hid), BF),
            jax.ShapeDtypeStruct((n_tp, hid, width), BF),
        ],
        in_specs=[ANY] * 5,
        out_specs=[ANY] * 5,
        scratch_shapes=[
            pltpu.VMEM((CAP, width), BF),
            pltpu.VMEM((positions, 2 * vdim), BF),
            pltpu.VMEM((width, hid), BF),
            pltpu.VMEM((hid, width), BF),
            sem((2, 3)), sem((2, 3)), sem((2, 3)), sem((2, 3)),
            sem((nz,)), sem((nz,)), sem((2,)), sem((2,)), sem((2,)), sem((2,)),
            sem((4,)), sem((4,)), sem((n_ep,)), sem((n_ep,)), sem((4,)),
        ],
        compiler_params=pltpu.CompilerParams(
            collective_id=0, has_side_effects=True, vmem_limit_bytes=8 * 1024 * 1024
        ),
        name="exchange",
    )(outgoing.reshape(n_ep, CAP, width), kv, w_gate[0], w_up[0], w_down[0])

    expert_out = pl.pallas_call(
        expert_kernel,
        grid=(n_tp,),
        out_shape=jax.ShapeDtypeStruct((slots, width), BF),
        in_specs=[
            pl.BlockSpec((slots, width), lambda g: (0, 0)),
            pl.BlockSpec((1, width, hid), lambda g: (g, 0, 0)),
            pl.BlockSpec((1, width, hid), lambda g: (g, 0, 0)),
            pl.BlockSpec((1, hid, width), lambda g: (g, 0, 0)),
        ],
        out_specs=pl.BlockSpec((slots, width), lambda g: (0, 0)),
        scratch_shapes=[pltpu.VMEM((slots, width), F32)],
        compiler_params=params(),
        cost_estimate=pl.CostEstimate(
            flops=6 * slots * width * hid * n_tp, bytes_accessed=16 * 1024 * 1024, transcendentals=0
        ),
        name="expert",
    )(arrived.reshape(slots, width), g_all, u_all, d_all)

    back = lax.all_to_all(
        expert_out.reshape(1, n_ep, CAP, width), "ep", split_axis=1, concat_axis=1, tiled=True
    )[0].reshape(slots, width)

    blk = 1024
    length = n_ep * positions
    attn_rows = pl.pallas_call(
        functools.partial(attention_kernel, blk),
        out_shape=jax.ShapeDtypeStruct((positions, heads * vdim), BF),
        in_specs=[VM, VM, pl.BlockSpec(memory_space=pltpu.SMEM), VM],
        out_specs=VM,
        scratch_shapes=[
            pltpu.VMEM((2 * heads, positions, vdim), BF),
            pltpu.VMEM((2 * heads, positions, 128), F32),
            pltpu.VMEM((2 * heads, positions, 2 * vdim), F32),
        ],
        compiler_params=params(),
        cost_estimate=pl.CostEstimate(
            flops=2 * 2 * heads * positions * length * 3 * vdim,
            bytes_accessed=length * 4 * vdim,
            transcendentals=2 * heads * positions * length,
        ),
        name="attend",
    )(
        jnp.transpose(queries, (1, 0, 2)),
        kv_all.reshape(length, 2 * vdim),
        attn_lambda,
        head_gain.reshape(1, vdim),
    )
    tiles = lax.all_to_all(
        attn_rows.reshape(n_tp, positions // n_tp, heads * vdim), "tp", 0, 0, tiled=True
    )
    mixer_out = jnp.einsum(
        "gsk,gkd->sd", tiles, w_out.reshape(n_tp, heads * vdim, width), preferred_element_type=F32
    ).astype(BF)

    moe_out = pl.pallas_call(
        combine_kernel,
        out_shape=jax.ShapeDtypeStruct((dev_rows, width), BF),
        in_specs=[VM, VM, VM],
        out_specs=VM,
        compiler_params=params(),
        name="combine",
    )(back, own_routes, own_weights)
    return (mixer_out, moe_out)


def solution(mesh):
    return jax.shard_map(
        local,
        mesh=mesh,
        in_specs=(
            P("ep", "tp", None),
            P("ep", "tp", None),
            P("ep", "tp", None),
            P("tp"),
            P(),
            P(),
            P("ep", None),
            P(),
            P("ep", None),
            P("ep", None),
            P("ep", None, "tp"),
            P("ep", None, "tp"),
            P("ep", "tp", None),
        ),
        out_specs=(P(("ep", "tp"), None), P(("ep", "tp"), None)),
        check_vma=False,
    )
```

```python
import functools

import jax
import jax.numpy as jnp
from jax import lax
from jax.experimental import pallas as pl
from jax.experimental.pallas import tpu as pltpu
from jax.sharding import PartitionSpec as P

EPSILON = 1e-06
MASKED = -1e30
MESH = pl.DeviceIdType.MESH
CAP = 8
BF = jnp.bfloat16
F32 = jnp.float32
ANY = pl.BlockSpec(memory_space=pl.ANY)
VM = pl.BlockSpec(memory_space=pltpu.VMEM)


def one_hot_slots(route_a, route_b, shape, token_dim, counts):
    slot_dim = 1 - token_dim
    slot = lax.broadcasted_iota(jnp.int32, shape, slot_dim)
    expert = slot // CAP
    place = (slot - expert * CAP).astype(F32)
    hit_a, hit_b = route_a == expert, route_b == expert
    hit = (hit_a | hit_b).astype(F32).astype(BF)
    earlier = counts(hit)
    here = earlier == place
    return hit_a & here, hit_b & here


def pack_kernel(rows_ref, gain_ref, routes_ref, out_ref):
    tokens = rows_ref.shape[0]
    slots = out_ref.shape[0]
    rows = rows_ref[...].astype(F32)
    mean_sq = jnp.mean(rows * rows, axis=-1, keepdims=True)
    normed = (rows * lax.rsqrt(mean_sq + EPSILON) * gain_ref[...]).astype(BF)
    before = (
        lax.broadcasted_iota(jnp.int32, (tokens, tokens), 0)
        < lax.broadcasted_iota(jnp.int32, (tokens, tokens), 1)
    )
    before = before.astype(F32).astype(BF)

    def counts(hit):
        return jnp.dot(hit, before, preferred_element_type=F32)

    first, second = one_hot_slots(
        routes_ref[0:1, :], routes_ref[1:2, :], (slots, tokens), 1, counts
    )
    pick = (first | second).astype(F32).astype(BF)
    step = 256
    for n in range(0, rows_ref.shape[1], step):
        out_ref[:, n : n + step] = jnp.dot(
            pick, normed[:, n : n + step], preferred_element_type=F32
        ).astype(BF)


def combine_kernel(back_ref, routes_ref, weights_ref, out_ref):
    tokens = out_ref.shape[0]
    slots = back_ref.shape[0]
    before = (
        lax.broadcasted_iota(jnp.int32, (tokens, tokens), 1)
        < lax.broadcasted_iota(jnp.int32, (tokens, tokens), 0)
    )
    before = before.astype(F32).astype(BF)

    def counts(hit):
        return jnp.dot(before, hit, preferred_element_type=F32)

    first, second = one_hot_slots(
        routes_ref[:, 0:1], routes_ref[:, 1:2], (tokens, slots), 0, counts
    )
    mix = jnp.where(first, weights_ref[:, 0:1], 0.0) + jnp.where(second, weights_ref[:, 1:2], 0.0)
    high = mix.astype(BF)
    low = (mix - high.astype(F32)).astype(BF)
    step = 256
    for n in range(0, out_ref.shape[1], step):
        part = back_ref[:, n : n + step]
        out_ref[:, n : n + step] = (
            jnp.dot(high, part, preferred_element_type=F32)
            + jnp.dot(low, part, preferred_element_type=F32)
        ).astype(BF)


def comm_kernel(
    n_ep, n_tp, nz, nx,
    slots_ref, kv_ref, wg_ref, wu_ref, wd_ref, q_ref, lam_ref, gain_ref,
    arrived_ref, g_ref, u_ref, d_ref, attn_ref,
    kv_all_ref, slot_tmp, w_tmp, wd_tmp, q_s, m_s, acc_s,
    w_send, w_recv, f_send, f_recv, z_send, z_recv, x_send, x_recv, y_send, y_recv,
    c_send, c_recv, d_send, d_recv, local_sem,
):
    me = lax.axis_index("ep")
    tp = lax.axis_index("tp")
    z = me // (2 * nx)
    x = (me // 2) % nx
    c = me % 2

    def ep_of(zz, xx, cc):
        return zz * (2 * nx) + xx * 2 + cc

    barrier = pltpu.get_barrier_semaphore()

    def greet(d, carry):
        pl.semaphore_signal(
            barrier, inc=1, device_id={"ep": lax.rem(me + d, n_ep)}, device_id_type=MESH
        )
        return carry

    lax.fori_loop(1, n_ep, greet, 0)
    for d in range(1, n_tp):
        pl.semaphore_signal(
            barrier, inc=1, device_id={"tp": lax.rem(tp + d, n_tp)}, device_id_type=MESH
        )
    pl.semaphore_wait(barrier, n_ep - 1 + n_tp - 1)

    def remote(src, dst, send, recv, where):
        return pltpu.make_async_remote_copy(
            src_ref=src, dst_ref=dst, send_sem=send, recv_sem=recv,
            device_id=where, device_id_type=MESH,
        )

    up, down = {"tp": lax.rem(tp + 1, n_tp)}, {"tp": lax.rem(tp + n_tp - 1, n_tp)}
    pairs = ((wg_ref, g_ref), (wu_ref, u_ref), (wd_ref, d_ref))

    def z_copy(k):
        to = ep_of(lax.rem(z + k, nz), x, c)
        return remote(kv_ref, kv_all_ref.at[z, x, c], z_send.at[k], z_recv.at[k], {"ep": to})

    for k in range(1, nz):
        z_copy(k).start()
    weights = []
    for i, (src, dst) in enumerate(pairs):
        for s, where in enumerate((up, down)):
            w = remote(src, dst.at[tp], w_send.at[s, i], w_recv.at[s, i], where)
            w.start()
            weights.append(w)

    def row_copy(d):
        to = lax.rem(me + d, n_ep)
        return remote(
            slots_ref.at[to], arrived_ref.at[me], d_send.at[d], d_recv.at[d], {"ep": to}
        )

    def row_start(d, carry):
        row_copy(d).start()
        return carry

    half = n_ep // 2
    lax.fori_loop(1, half, row_start, 0)

    def stay(src, tmp, dst, n):
        pull = pltpu.make_async_copy(src, tmp, local_sem.at[n])
        pull.start()
        pull.wait()
        push = pltpu.make_async_copy(tmp, dst, local_sem.at[n])
        push.start()
        push.wait()

    own_kv = pltpu.make_async_copy(kv_ref, kv_all_ref.at[z, x, c], local_sem.at[0])
    own_kv.start()
    own_kv.wait()
    stay(slots_ref.at[me], slot_tmp, arrived_ref.at[me], 1)
    stay(wg_ref, w_tmp, g_ref.at[tp], 2)
    stay(wu_ref, w_tmp, u_ref.at[tp], 2)
    stay(wd_ref, wd_tmp, d_ref.at[tp], 3)

    for k in range(1, nz):
        z_copy(k).wait()

    xr, xl = lax.rem(x + 1, nx), lax.rem(x + nx - 1, nx)
    x2 = lax.rem(x + 2, nx)
    right, left = {"ep": ep_of(z, xr, c)}, {"ep": ep_of(z, xl, c)}
    twin = {"ep": ep_of(z, x, 1 - c)}

    def column(xx):
        return kv_all_ref.at[:, xx, c]

    def across(n, xx):
        return remote(column(xx), column(xx), c_send.at[n], c_recv.at[n], twin)

    to_right = remote(column(x), column(x), x_send.at[0], x_recv.at[0], right)
    to_left = remote(column(x), column(x), x_send.at[1], x_recv.at[1], left)
    to_right.start()
    to_left.start()
    across(0, x).start()
    lax.fori_loop(half, n_ep, row_start, 0)

    def forward(i):
        src, dst = pairs[i]
        mid = src.shape[0] // 2
        came_up, came_down = lax.rem(tp + n_tp - 1, n_tp), lax.rem(tp + 1, n_tp)
        low, high = pl.ds(0, mid), pl.ds(mid, mid)
        return (
            remote(dst.at[came_up, low], dst.at[came_up, low], f_send.at[0, i], f_recv.at[0, i], up),
            remote(
                dst.at[came_down, high], dst.at[came_down, high], f_send.at[1, i], f_recv.at[1, i], down
            ),
        )

    def pass_on(i):
        for w in weights[2 * i : 2 * i + 2]:
            w.wait_recv()
        for f in forward(i):
            f.start()

    pass_on(0)
    pass_on(1)

    to_right.wait_recv()
    hz = nz // 2
    on_right = remote(
        kv_all_ref.at[pl.ds(0, hz), xl, c], kv_all_ref.at[pl.ds(0, hz), xl, c],
        y_send.at[0], y_recv.at[0], right,
    )
    on_right.start()
    across(1, xl).start()
    to_left.wait_recv()
    on_left = remote(
        kv_all_ref.at[pl.ds(hz, hz), xr, c], kv_all_ref.at[pl.ds(hz, hz), xr, c],
        y_send.at[1], y_recv.at[1], left,
    )
    on_left.start()
    across(2, xr).start()
    pass_on(2)
    on_right.wait_recv()
    on_left.wait_recv()
    across(3, x2).start()
    for n, xx in enumerate((x, xl, xr, x2)):
        across(n, xx).wait()
    n_pos = kv_ref.shape[0]

    def kv_block(b):
        pieces = [
            kv_all_ref[b // (nx // 2), 2 * lax.rem(b, nx // 2) + j // 2, j % 2] for j in range(4)
        ]
        return jnp.concatenate(pieces, axis=0)

    attend(me, 4 * n_pos, q_ref, kv_block, lam_ref, gain_ref, attn_ref, q_s, m_s, acc_s)

    def row_wait(d, carry):
        row_copy(d).wait()
        return carry

    lax.fori_loop(1, n_ep, row_wait, 0)
    for w in weights:
        w.wait_send()
    for i in range(3):
        for f in forward(i):
            f.wait()
    for w in (to_right, to_left, on_right, on_left):
        w.wait_send()


def expert_kernel(rows_ref, g_ref, u_ref, d_ref, out_ref, acc_ref):
    g = pl.program_id(0)

    @pl.when(g == 0)
    def _():
        acc_ref[...] = jnp.zeros_like(acc_ref)

    step = 256
    for m in range(0, rows_ref.shape[0], step):
        rows = rows_ref[m : m + step, :]
        gate = jnp.dot(rows, g_ref[0], preferred_element_type=F32)
        upper = jnp.dot(rows, u_ref[0], preferred_element_type=F32)
        hidden = (gate / (1.0 + jnp.exp(-gate)) * upper).astype(BF)
        for n in range(0, out_ref.shape[1], 512):
            part = jnp.dot(hidden, d_ref[0, :, n : n + 512], preferred_element_type=F32)
            acc_ref[m : m + step, n : n + 512] += part.astype(BF).astype(F32)

    @pl.when(g == pl.num_programs(0) - 1)
    def _():
        out_ref[...] = acc_ref[...].astype(BF)


def attend(me, blk, q_ref, kv_block, lam_ref, gain_ref, out_ref, q_s, m_s, acc_s):
    rows = q_ref.shape[1]
    heads = q_ref.shape[0]
    vdim = q_ref.shape[2]
    hd = vdim // 2
    lane = lax.broadcasted_iota(jnp.int32, (rows, vdim), 1)
    for h in range(heads):
        q = q_ref[h] * jnp.asarray(hd**-0.5, BF)
        for m in range(2):
            q_s[2 * h + m] = jnp.where((lane // hd) == m, q, jnp.zeros_like(q))
    m_s[...] = jnp.full_like(m_s, MASKED)
    acc_s[...] = jnp.zeros_like(acc_s)

    def block(b, masked):
        start = pl.multiple_of(b * blk, blk)
        kv = kv_block(b)
        k, v = kv[:, 0:vdim], kv[:, vdim : 2 * vdim]
        v_one = jnp.concatenate([v, jnp.ones_like(v)], axis=1)
        for r in range(2 * heads):
            s = lax.dot_general(
                q_s[r], k, (((1,), (1,)), ((), ())), preferred_element_type=F32
            )
            if masked:
                kp = start + lax.broadcasted_iota(jnp.int32, s.shape, 1)
                qp = me * rows + lax.broadcasted_iota(jnp.int32, s.shape, 0)
                s = jnp.where(kp <= qp, s, MASKED)
            old = m_s[r]
            new = jnp.maximum(old, jnp.max(s, axis=1, keepdims=True))
            shrink = jnp.exp(old - new)
            p = jnp.exp(s - new[:, 0:1]).astype(BF)
            m_s[r] = new
            acc_s[r] = acc_s[r] * shrink[:, 0:1] + jnp.dot(p, v_one, preferred_element_type=F32)

    last = (me * rows) // blk

    def body(b, carry):
        block(b, False)
        return carry

    lax.fori_loop(0, last, body, 0)
    block(last, True)
    for h in range(heads):
        ratio = [acc_s[2 * h + m][:, 0:vdim] / acc_s[2 * h + m][:, vdim:] for m in range(2)]
        out = ratio[0] - lam_ref[h] * ratio[1]
        mean_sq = jnp.mean(out * out, axis=-1, keepdims=True)
        out_ref[:, h * vdim : (h + 1) * vdim] = (
            out * lax.rsqrt(mean_sq + EPSILON) * gain_ref[...]
        ).astype(BF)


def params(**kw):
    return pltpu.CompilerParams(vmem_limit_bytes=48 * 1024 * 1024, **kw)


def local(
    queries, keys, values, attn_lambda, head_gain, w_out,
    moe_rows, moe_gain, routes, route_weights, w_gate, w_up, w_down,
):
    n_ep, n_tp = lax.axis_size("ep"), lax.axis_size("tp")
    nx = 4
    nz = n_ep // (2 * nx)
    tp = lax.axis_index("tp")
    positions, heads, vdim = queries.shape
    width = moe_rows.shape[1]
    dev_rows = moe_rows.shape[0] // n_tp
    slots = n_ep * CAP
    hid = w_gate.shape[2]

    own_rows = lax.dynamic_slice_in_dim(moe_rows, tp * dev_rows, dev_rows, 0)
    own_routes = lax.dynamic_slice_in_dim(routes, tp * dev_rows, dev_rows, 0)
    own_weights = lax.dynamic_slice_in_dim(route_weights, tp * dev_rows, dev_rows, 0)

    outgoing = pl.pallas_call(
        pack_kernel,
        out_shape=jax.ShapeDtypeStruct((slots, width), BF),
        in_specs=[VM, VM, VM],
        out_specs=VM,
        compiler_params=params(),
        name="pack",
    )(own_rows, moe_gain.reshape(1, width), own_routes.T)

    kv = jnp.concatenate([keys[:, 0], values[:, 0]], axis=1)
    sem = pltpu.SemaphoreType.DMA
    arrived, g_all, u_all, d_all, attn_rows = pl.pallas_call(
        functools.partial(comm_kernel, n_ep, n_tp, nz, nx),
        out_shape=[
            jax.ShapeDtypeStruct((n_ep, CAP, width), BF),
            jax.ShapeDtypeStruct((n_tp, width, hid), BF),
            jax.ShapeDtypeStruct((n_tp, width, hid), BF),
            jax.ShapeDtypeStruct((n_tp, hid, width), BF),
            jax.ShapeDtypeStruct((positions, heads * vdim), BF),
        ],
        in_specs=[ANY] * 5 + [VM, pl.BlockSpec(memory_space=pltpu.SMEM), VM],
        out_specs=[ANY] * 4 + [VM],
        scratch_shapes=[
            pltpu.VMEM((nz, nx, 2, positions, 2 * vdim), BF),
            pltpu.VMEM((CAP, width), BF),
            pltpu.VMEM((width, hid), BF),
            pltpu.VMEM((hid, width), BF),
            pltpu.VMEM((2 * heads, positions, vdim), BF),
            pltpu.VMEM((2 * heads, positions, 128), F32),
            pltpu.VMEM((2 * heads, positions, 2 * vdim), F32),
            sem((2, 3)), sem((2, 3)), sem((2, 3)), sem((2, 3)),
            sem((nz,)), sem((nz,)), sem((2,)), sem((2,)), sem((2,)), sem((2,)),
            sem((4,)), sem((4,)), sem((n_ep,)), sem((n_ep,)), sem((4,)),
        ],
        compiler_params=pltpu.CompilerParams(
            collective_id=0, has_side_effects=True, vmem_limit_bytes=56 * 1024 * 1024
        ),
        name="exchange",
    )(
        outgoing.reshape(n_ep, CAP, width), kv, w_gate[0], w_up[0], w_down[0],
        jnp.transpose(queries, (1, 0, 2)), attn_lambda, head_gain.reshape(1, vdim),
    )

    expert_out = pl.pallas_call(
        expert_kernel,
        grid=(n_tp,),
        out_shape=jax.ShapeDtypeStruct((slots, width), BF),
        in_specs=[
            pl.BlockSpec((slots, width), lambda g: (0, 0)),
            pl.BlockSpec((1, width, hid), lambda g: (g, 0, 0)),
            pl.BlockSpec((1, width, hid), lambda g: (g, 0, 0)),
            pl.BlockSpec((1, hid, width), lambda g: (g, 0, 0)),
        ],
        out_specs=pl.BlockSpec((slots, width), lambda g: (0, 0)),
        scratch_shapes=[pltpu.VMEM((slots, width), F32)],
        compiler_params=params(),
        cost_estimate=pl.CostEstimate(
            flops=6 * slots * width * hid * n_tp, bytes_accessed=16 * 1024 * 1024, transcendentals=0
        ),
        name="expert",
    )(arrived.reshape(slots, width), g_all, u_all, d_all)

    back = lax.all_to_all(
        expert_out.reshape(1, n_ep, CAP, width), "ep", split_axis=1, concat_axis=1, tiled=True
    )[0].reshape(slots, width)

    tiles = lax.all_to_all(
        attn_rows.reshape(n_tp, positions // n_tp, heads * vdim), "tp", 0, 0, tiled=True
    )
    mixer_out = jnp.einsum(
        "gsk,gkd->sd", tiles, w_out.reshape(n_tp, heads * vdim, width), preferred_element_type=F32
    ).astype(BF)

    moe_out = pl.pallas_call(
        combine_kernel,
        out_shape=jax.ShapeDtypeStruct((dev_rows, width), BF),
        in_specs=[VM, VM, VM],
        out_specs=VM,
        compiler_params=params(),
        name="combine",
    )(back, own_routes, own_weights)
    return (mixer_out, moe_out)


def solution(mesh):
    return jax.shard_map(
        local,
        mesh=mesh,
        in_specs=(
            P("ep", "tp", None),
            P("ep", "tp", None),
            P("ep", "tp", None),
            P("tp"),
            P(),
            P(),
            P("ep", None),
            P(),
            P("ep", None),
            P("ep", None),
            P("ep", None, "tp"),
            P("ep", None, "tp"),
            P("ep", "tp", None),
        ),
        out_specs=(P(("ep", "tp"), None), P(("ep", "tp"), None)),
        check_vma=False,
    )
```
